32 devices in a mesh: ep: 8 (over z, y), tp: 4 (over x, core).
Axes of the slice: x: 2, y: 2, z: 4, core: 2. Of those that a mesh axis runs over, the one named last changes fastest.
Arguments:
- mixer_input: bfloat16 [4096, 2048], P(('ep', 'tp')), may hold values from -6 to 6
- expert_input: bfloat16 [4096, 2048], P(('ep', 'tp')), may hold values from -6 to 6
- mixer_gain: float32 [2048], replicated, may hold values from 0.1 to 1.9
- expert_gain: float32 [2048], replicated, may hold values from 0.1 to 1.9
- query_weight: bfloat16 [2048, 1024], P(None, 'tp'), may hold values from -0.125 to 0.125
- key_weight: bfloat16 [2048, 1024], P(None, 'tp'), may hold values from -0.125 to 0.125
- value_weight: bfloat16 [2048, 1024], P(None, 'tp'), may hold values from -0.125 to 0.125
- out_weight: bfloat16 [1024, 2048], P('tp'), may hold values from -0.1875 to 0.1875
- decay_rate: float32 [8], P('tp'), may hold values from 0 to 0.12
- routing: int32 [4096, 4], P('ep'), may hold values from 0 to 7, all different within a row; in each aligned block of 128 rows (0 to 127, 128 to 255, ...) at most 96 rows name the same one
- route_weight: float32 [4096, 4], P('ep'), may hold values from 0.2 to 1
- gate_weight: bfloat16 [8, 2048, 1024], P('ep', None, 'tp'), may hold values from -0.125 to 0.125
- up_weight: bfloat16 [8, 2048, 1024], P('ep', None, 'tp'), may hold values from -0.125 to 0.125
- down_weight: bfloat16 [8, 1024, 2048], P('ep', None, 'tp'), may hold values from -0.1875 to 0.1875
- shared_gate: bfloat16 [2048, 512], P(None, 'tp'), may hold values from -0.125 to 0.125
- shared_up: bfloat16 [2048, 512], P(None, 'tp'), may hold values from -0.125 to 0.125
- shared_down: bfloat16 [512, 2048], P(None, 'tp'), may hold values from -0.25 to 0.25
Outputs:
- mixer_output: float32 [4096, 2048], P(('ep', 'tp'))
- expert_output: float32 [4096, 2048], P('ep', 'tp')
The draws below stay inside these ranges and needn't reach their ends.
Inputs may be any that keep to these rules, and one draw needn't show every extreme that they name: `routing`: each row names 4 different experts. In each aligned block of 128 rows, no expert is named by more than 96 rows, and in some blocks one expert is named by exactly 96 rows.
All inputs are finite; a program needn't handle non-finite values.
Results may differ from the reference program's by a relative error of at most 0.0095.
Values may be sent and summed in bfloat16 or wider, within the bound.
A program may use at most 128 MiB of HBM per device.

```python
import math
import jax
import jax.numpy as jnp
import numpy as np
from jax import lax

D = 2048
HEADS = 8
HD = 128
F = 1024
FS = 512
K = 4
BLK = 64
R = 128
TOKENS = 4096
EXPERTS = 8
CAP = 96
N_EP = 8
N_TP = 4


def draw_decay_rate(key, part):
    order_key = jax.random.fold_in(key, 11)
    slow_key = jax.random.fold_in(key, 12)
    fast_key = jax.random.fold_in(key, 13)
    ranking = jax.random.permutation(order_key, HEADS)
    fast_count = HEADS // 2
    is_fast = ranking < fast_count
    slow_rate = jnp.exp(jax.random.uniform(slow_key, (HEADS,), jnp.float32, math.log(0.05), 0.0)) * (math.log(10.0) / TOKENS)
    quick_decay_rate = jax.random.uniform(fast_key, (HEADS,), jnp.float32, 0.05, 0.12)
    return jnp.where(is_fast, quick_decay_rate, slow_rate).astype(jnp.float32)


def block_levels(key, extent, split, low, top_value):
    gain, own = 1.0, jax.random.fold_in(key, 6)
    for position, shards_of in split:
        heights = jnp.exp(jax.random.uniform(jax.random.fold_in(own, position), (shards_of,), jnp.float32, low / len(split), top_value / len(split)))
        gain = gain * jnp.repeat(heights, extent[position] // shards_of).reshape([-1 if axis == position else 1 for axis in range(len(extent))])
    return gain


def assign_block(rng, own, number, rows, count, top, bound, skew):
    order = jax.random.permutation(rng, count)
    heavy_load, ordinary = shares(count, rows * top, bound, skew, True), shares(count, rows * top, bound, skew, False)
    places = jnp.arange(count)

    def named(tallies, rotation):
        used = int((tallies > 0).sum())
        fixed = max(1, used // 4)
        moved = fixed + (places - fixed + rotation * (used - fixed)) % max(1, count - fixed)
        return jnp.zeros((count,), jnp.int32).at[order[jnp.where(places < fixed, places, moved)]].set(jnp.asarray(tallies, jnp.int32))

    tallies = jnp.where(number % 4 == 0, named(heavy_load, number // 4), named(ordinary, number - number // 4 - 1))
    mixed = jax.random.permutation(jax.random.fold_in(own, 3), count)
    source_of, receiver = mixed[0:count // 2 * 2:2], mixed[1:count // 2 * 2:2]
    margin = jnp.minimum(tallies[source_of] - 1, bound - tallies[receiver]) // 2
    margin = jnp.where((source_of == order[0]) | (receiver == order[0]) | (tallies[receiver] == 0), 0, jnp.maximum(margin, 0))
    moved = jax.random.randint(jax.random.fold_in(own, 4), (count // 2,), 0, 1 << 20) % (margin + 1)
    tallies = tallies.at[source_of].add(-moved).at[receiver].add(moved)
    items = jnp.searchsorted(jnp.cumsum(tallies), jnp.arange(rows * top), side="right").astype(jnp.int32)
    grid = items.reshape(top, rows).T
    grid = grid[jax.random.permutation(jax.random.fold_in(own, 1), rows)]
    rotation = jax.random.randint(jax.random.fold_in(own, 2), (rows, 1), 0, top)
    return jnp.take_along_axis(grid, (jnp.arange(top)[None, :] + rotation) % top, axis=1)


def shares(number_of, total, bound, skew, full):
    portions = [(1 << 20) // math.isqrt(grade ** skew) + 1 for grade in range(1, number_of + 1)]
    largest = bound if full else min(bound, max(-(-total // number_of), total * portions[0] // sum(portions)))
    least = 1 if total - largest >= number_of - 1 else 0
    counts, rest = [largest] + [least] * (number_of - 1), total - largest - least * (number_of - 1)
    while rest > 0:
        movable = [i for i in range(1, number_of) if counts[i] < largest] or [i for i in range(1, number_of) if counts[i] < bound]
        mass, budget = sum([portions[i] for i in movable]), rest
        for i in movable:
            more = min(bound - counts[i], max(1, budget * portions[i] // mass), rest)
            counts[i] = counts[i] + more
            rest = rest - more
    return np.array(counts)


def gaussian(key, dims, spread, most, shards=(), kind=jnp.bfloat16):
    array = jax.random.normal(key, dims, jnp.float32) * spread
    if len(shards) > 0:
        array = block_levels(key, dims, shards, -0.22, 0.18) * array
    return jnp.clip(array, min=-most, max=most).astype(kind)


def setup_inputs(seed: int = 0) -> dict:
    key_list = jax.random.split(jax.random.key(seed), 18)
    mixer_input = gaussian(key_list[0], (TOKENS, D), 1.0, 6.0, ((0, 32),))
    expert_input = gaussian(key_list[1], (TOKENS, D), 1.0, 6.0, ((0, 32),))
    mixer_gain = jnp.clip(1.0 + 0.18 * jax.random.normal(key_list[2], (D,), jnp.float32), 0.1, 1.9)
    expert_gain = jnp.clip(1.0 + 0.18 * jax.random.normal(key_list[3], (D,), jnp.float32), 0.1, 1.9)
    query_weight = gaussian(key_list[4], (D, HEADS * HD), D ** -0.5, 0.125, ((1, 4),))
    key_weight = gaussian(key_list[5], (D, HEADS * HD), D ** -0.5, 0.125, ((1, 4),))
    value_weight = gaussian(key_list[6], (D, HEADS * HD), D ** -0.5, 0.125, ((1, 4),))
    out_weight = gaussian(key_list[7], (HEADS * HD, D), (HEADS * HD) ** -0.5, 0.1875, ((0, 4),))
    decay_rate = draw_decay_rate(jax.random.fold_in(key_list[17], 71), 0)
    routing_keys = jax.random.split(jax.random.fold_in(key_list[9], 1), TOKENS // R)
    routing_turns = jax.random.permutation(jax.random.fold_in(key_list[9], 3), TOKENS // R)
    routing = jax.vmap(lambda own, number: assign_block(jax.random.fold_in(key_list[9], 2), own, number, R, EXPERTS, K, CAP, 1))(routing_keys, routing_turns).reshape((TOKENS, K))
    route_weight = jnp.clip(0.2 + 0.8 * jax.random.uniform(key_list[10], (TOKENS, K), jnp.float32) ** block_levels(key_list[10], (TOKENS, K), ((0, 8),), -0.2, 0.2), 0.2, 1.0)
    gate_weight = gaussian(key_list[11], (EXPERTS, D, F), D ** -0.5, 0.125, ((0, 8), (2, 4)))
    up_weight = gaussian(key_list[12], (EXPERTS, D, F), D ** -0.5, 0.125, ((0, 8), (2, 4)))
    down_weight = gaussian(key_list[13], (EXPERTS, F, D), F ** -0.5, 0.1875, ((0, 8), (2, 4)))
    shared_gate = gaussian(key_list[14], (D, FS), D ** -0.5, 0.125, ((1, 4),))
    shared_up = gaussian(key_list[15], (D, FS), D ** -0.5, 0.125, ((1, 4),))
    shared_down = gaussian(key_list[16], (FS, D), FS ** -0.5, 0.25, ((1, 4),))
    return dict(mixer_input=mixer_input, expert_input=expert_input, mixer_gain=mixer_gain, expert_gain=expert_gain, query_weight=query_weight, key_weight=key_weight, value_weight=value_weight, out_weight=out_weight, decay_rate=decay_rate, routing=routing, route_weight=route_weight, gate_weight=gate_weight, up_weight=up_weight, down_weight=down_weight, shared_gate=shared_gate, shared_up=shared_up, shared_down=shared_down)


NORM_EPS = 1e-06
ROPE_BASE = 10000.0
EXACT_MATMUL = lax.Precision.HIGHEST

def norm_rows(inputs, gain_vector):
    values = inputs.astype(jnp.float32)
    scaled = values * lax.rsqrt(lax.optimization_barrier(jnp.mean(values * values, axis=-1, keepdims=True)) + NORM_EPS)
    return (scaled * gain_vector.astype(jnp.float32)).astype(jnp.bfloat16)

def rotate(head_rows, positions):
    head_size = head_rows.shape[-1]
    inverse = ROPE_BASE ** (-jnp.arange(0, head_size, 2, dtype=jnp.float32) / head_size)
    angles = positions[:, None] * inverse[None, :]
    cosine = jnp.cos(angles)[:, None, :]
    sine_part = jnp.sin(angles)[:, None, :]
    front_half = head_rows[..., :head_size // 2]
    behind = head_rows[..., head_size // 2:]
    return jnp.concatenate([front_half * cosine - behind * sine_part, front_half * sine_part + behind * cosine], axis=-1)

def project(inputs, weight):
    product = jnp.dot(inputs, weight, preferred_element_type=jnp.float32).astype(jnp.bfloat16)
    product = lax.optimization_barrier(product)
    return product.astype(jnp.float32).reshape(inputs.shape[0], HEADS, HD)

def retention_scan(query_heads, key_heads, value_heads, decay_rates):
    length = query_heads.shape[0]
    blocks = length // BLK
    log_gamma = -decay_rates.astype(jnp.float32)
    inner_pos = jnp.arange(BLK, dtype=jnp.float32)
    offsets = inner_pos[:, None] - inner_pos[None, :]
    inside_block_output = jnp.where(offsets >= 0, jnp.exp(log_gamma[:, None, None] * jnp.maximum(offsets, 0.0)), 0.0)
    key_scale = jnp.exp(log_gamma[None, :] * (BLK - 1.0 - inner_pos)[:, None])
    query_scale = jnp.exp(log_gamma[None, :] * (inner_pos + 1.0)[:, None])
    through = jnp.exp(log_gamma * BLK)

    def advance(carried, block_in):
        query_block_slice, key_block_slice, v_block = block_in
        attention_scores = jnp.einsum('ayr,iyr->yai', query_block_slice, key_block_slice, precision=EXACT_MATMUL) * inside_block_output
        nearby = jnp.einsum('hcm,mhe->che', attention_scores, v_block, precision=EXACT_MATMUL)
        distant = jnp.einsum('chd,hde->che', query_block_slice * query_scale[:, :, None], carried, precision=EXACT_MATMUL)
        update = jnp.einsum('chd,che->hde', key_block_slice * key_scale[:, :, None], v_block, precision=EXACT_MATMUL)
        return (through[:, None, None] * carried + update, nearby + distant)
    blocked = (blocks, BLK, HEADS, HD)
    _, outputs = lax.scan(advance, jnp.zeros((HEADS, HD, HD), jnp.float32), (query_heads.reshape(blocked), key_heads.reshape(blocked), value_heads.reshape(blocked)))
    return outputs.reshape(length, HEADS, HD)

def reference(mixer_input, expert_input, mixer_gain, expert_gain, query_weight, key_weight, value_weight, out_weight, decay_rate, routing, route_weight, gate_weight, up_weight, down_weight, shared_gate, shared_up, shared_down):
    mixer_rows = norm_rows(mixer_input, mixer_gain)
    positions = jnp.arange(TOKENS, dtype=jnp.float32)
    query_heads = rotate(project(mixer_rows, query_weight), positions) * HD ** (-0.5)
    key_heads = rotate(project(mixer_rows, key_weight), positions)
    value_heads = project(mixer_rows, value_weight)
    retained = retention_scan(query_heads, key_heads, value_heads, decay_rate)
    normed = retained * lax.rsqrt(lax.optimization_barrier(jnp.mean(retained * retained, axis=-1, keepdims=True)) + NORM_EPS)
    mixed_heads = normed.astype(jnp.bfloat16).reshape(TOKENS, HEADS * HD)
    group_width = HEADS * HD // N_TP
    summed_out = jnp.zeros((TOKENS, D), jnp.float32)
    for group_id in range(N_TP):
        partial_out = jnp.dot(mixed_heads[:, group_id * group_width:(group_id + 1) * group_width], out_weight[group_id * group_width:(group_id + 1) * group_width], preferred_element_type=jnp.float32).astype(jnp.bfloat16)
        summed_out = summed_out + lax.optimization_barrier(partial_out).astype(jnp.float32)
    mixer_output = summed_out
    expert_rows = norm_rows(expert_input, expert_gain)
    assigned = TOKENS * K
    chosen = routing.reshape(assigned).astype(jnp.int32)
    onehot = (chosen[:, None] == jnp.arange(EXPERTS, dtype=jnp.int32)[None, :]).astype(jnp.int32)
    ranks = lax.optimization_barrier(jnp.sum((jnp.cumsum(onehot, axis=0) - onehot) * onehot, axis=1)).astype(jnp.int32)
    owners = (jnp.arange(assigned, dtype=jnp.int32) // K + 1).astype(jnp.int32)
    room_size = N_EP * N_TP * CAP
    owner_table = jnp.zeros((EXPERTS, room_size), jnp.int32).at[chosen, ranks].set(owners)
    weight_table = jnp.zeros((EXPERTS, room_size), jnp.float32).at[chosen, ranks].set(route_weight.reshape(assigned).astype(jnp.float32))
    padded = jnp.concatenate([jnp.zeros((1, D), jnp.bfloat16), expert_rows], axis=0)

    def one_expert(summed, inputs):
        owner_ids, scales, gate_part, up_part, down_part = inputs
        picked = padded[owner_ids]
        hidden = (jax.nn.silu(jnp.dot(picked, gate_part, preferred_element_type=jnp.float32)) * jnp.dot(picked, up_part, preferred_element_type=jnp.float32)).astype(jnp.bfloat16)
        result = jnp.dot(hidden, down_part, preferred_element_type=jnp.float32).astype(jnp.bfloat16)
        result = lax.optimization_barrier(result).astype(jnp.float32)
        return (summed.at[owner_ids].add(result * scales[:, None]), None)
    summed, _ = lax.scan(one_expert, jnp.zeros((TOKENS + 1, D), jnp.float32), (owner_table, weight_table, gate_weight, up_weight, down_weight))
    shared_hidden = (jax.nn.silu(jnp.dot(expert_rows, shared_gate, preferred_element_type=jnp.float32)) * jnp.dot(expert_rows, shared_up, preferred_element_type=jnp.float32)).astype(jnp.bfloat16)
    shared_result = jnp.dot(shared_hidden, shared_down, preferred_element_type=jnp.float32)
    expert_output = summed[1:] + shared_result
    return (mixer_output, expert_output)
```

```python
import jax
import jax.numpy as jnp
from jax import lax
from jax.sharding import PartitionSpec as P

HD = 128


NORM_EPS = 1e-06
ROPE_BASE = 10000.0


def norm_rows(inputs, gain_vector):
    values = inputs.astype(jnp.float32)
    scaled = values * lax.rsqrt(jnp.mean(values * values, axis=-1, keepdims=True) + NORM_EPS)
    return (scaled * gain_vector).astype(jnp.bfloat16)


def rotate(head_rows, positions):
    head_size = head_rows.shape[-1]
    inverse = ROPE_BASE ** (-jnp.arange(0, head_size, 2, dtype=jnp.float32) / head_size)
    angles = positions[:, None] * inverse[None, :]
    cosine = jnp.cos(angles)[:, None, :]
    sine_part = jnp.sin(angles)[:, None, :]
    front_half = head_rows[..., : head_size // 2]
    behind = head_rows[..., head_size // 2 :]
    return jnp.concatenate(
        [front_half * cosine - behind * sine_part, front_half * sine_part + behind * cosine],
        axis=-1,
    )


def project(inputs, weight, head_total):
    product = jnp.dot(inputs, weight, preferred_element_type=jnp.float32).astype(jnp.bfloat16)
    product = lax.optimization_barrier(product)
    return product.astype(jnp.float32).reshape(inputs.shape[0], head_total, -1)


def retain_local(query_heads, key_heads, value_heads, decay_rates):
    length, head_total, head_size = query_heads.shape
    narrow = jnp.bfloat16
    log_gamma = -decay_rates
    place = lax.axis_index("ep")
    inner_pos = jnp.arange(length, dtype=jnp.float32)
    key_scale = jnp.exp(log_gamma[None, :] * (length - 1.0 - inner_pos)[:, None])
    summary = jnp.einsum(
        "nhd,nhe->hde",
        (key_heads * key_scale[:, :, None]).astype(narrow),
        value_heads.astype(narrow),
        preferred_element_type=jnp.float32,
    )
    gathered = lax.all_gather(summary, "ep")
    gaps = (place - 1 - jnp.arange(gathered.shape[0])).astype(jnp.float32)
    mix = jnp.where(
        gaps[:, None] >= 0,
        jnp.exp(log_gamma[None, :] * length * jnp.maximum(gaps, 0.0)[:, None]),
        0.0,
    )
    incoming = jnp.sum(mix[:, :, None, None] * gathered, axis=0)
    offsets = inner_pos[:, None] - inner_pos[None, :]
    decay_mask = jnp.where(
        offsets >= 0, jnp.exp(log_gamma[:, None, None] * jnp.maximum(offsets, 0.0)), 0.0
    )
    scores = (
        jnp.einsum(
            "nhd,mhd->hnm",
            query_heads.astype(narrow),
            key_heads.astype(narrow),
            preferred_element_type=jnp.float32,
        )
        * decay_mask
    )
    nearby = jnp.einsum(
        "hnm,mhe->nhe",
        scores.astype(narrow),
        value_heads.astype(narrow),
        preferred_element_type=jnp.float32,
    )
    query_scale = jnp.exp(log_gamma[None, :] * (inner_pos + 1.0)[:, None])
    distant = jnp.einsum(
        "nhd,hde->nhe",
        (query_heads * query_scale[:, :, None]).astype(narrow),
        incoming.astype(narrow),
        preferred_element_type=jnp.float32,
    )
    retained = nearby + distant
    normed = retained * lax.rsqrt(jnp.mean(retained * retained, axis=-1, keepdims=True) + NORM_EPS)
    return normed.astype(jnp.bfloat16).reshape(length, head_total * head_size)


def assign_slots(routes, source_rows, capacity, expert_count):
    token_count, pick_count = routes.shape
    chosen = routes.reshape(token_count * pick_count)
    onehot = (chosen[:, None] == jnp.arange(expert_count, dtype=jnp.int32)[None, :]).astype(
        jnp.int32
    )
    per_source = onehot.reshape(token_count // source_rows, source_rows * pick_count, expert_count)
    earlier_hits = jnp.cumsum(per_source, axis=1) - per_source
    ranks = jnp.sum(earlier_hits * per_source, axis=2).reshape(token_count * pick_count)
    sources = jnp.arange(token_count * pick_count, dtype=jnp.int32) // (source_rows * pick_count)
    return (chosen, sources * capacity + ranks)


def gather_slots(token_rows, chosen, slot_ids, slot_count, expert_count, pick_count):
    owners = jnp.arange(chosen.shape[0], dtype=jnp.int32) // pick_count + 1
    owner_table = jnp.zeros((slot_count, expert_count), jnp.int32).at[slot_ids, chosen].set(owners)
    padded = jnp.concatenate(
        [jnp.zeros((1, token_rows.shape[1]), token_rows.dtype), token_rows], axis=0
    )
    return padded[owner_table]


def expert_hidden(routed_rows, gate_weight, up_weight):
    per_device = gate_weight.shape[0]
    grouped = routed_rows.reshape(
        routed_rows.shape[0], routed_rows.shape[1] // per_device, per_device, routed_rows.shape[2]
    )
    gate_part = jnp.einsum(
        "snxd,xdf->snxf", grouped, gate_weight, preferred_element_type=jnp.float32
    )
    up_part = jnp.einsum("snxd,xdf->snxf", grouped, up_weight, preferred_element_type=jnp.float32)
    return (jax.nn.silu(gate_part) * up_part).astype(jnp.bfloat16)


def routed_dense(own_rows, routing, route_weight, gate_weight, up_weight, down_weight):
    own_count = own_rows.shape[0]
    local_experts = gate_weight.shape[0]
    expert_count = lax.axis_size("ep") * local_experts
    start = lax.axis_index("tp") * own_count
    own_routing = lax.dynamic_slice_in_dim(routing, start, own_count, 0)
    own_weight = lax.dynamic_slice_in_dim(route_weight, start, own_count, 0)
    named = own_routing[:, :, None] == jnp.arange(expert_count, dtype=jnp.int32)
    spread = jnp.sum(jnp.where(named, own_weight[:, :, None], 0.0), axis=1)
    rows = lax.all_gather(own_rows, "ep", axis=0, tiled=True)
    gate_all = lax.all_gather(gate_weight, "tp", axis=0)
    up_all = lax.all_gather(up_weight, "tp", axis=0)
    down_all = lax.all_gather(down_weight, "tp", axis=0)
    scales = lax.all_gather(spread, "ep", axis=0, tiled=True)
    scales = lax.dynamic_slice_in_dim(
        scales, lax.axis_index("ep") * local_experts, local_experts, 1
    )
    parts = gate_all.shape[0]
    total = None
    for x in range(local_experts):
        hidden = jnp.concatenate(
            [
                (
                    jax.nn.silu(jnp.dot(rows, gate_all[p, x], preferred_element_type=jnp.float32))
                    * jnp.dot(rows, up_all[p, x], preferred_element_type=jnp.float32)
                ).astype(jnp.bfloat16)
                for p in range(parts)
            ],
            axis=1,
        )
        result = jnp.concatenate(
            [
                jnp.dot(hidden, down_all[p, x], preferred_element_type=jnp.float32)
                * scales[:, x : x + 1]
                for p in range(parts)
            ],
            axis=1,
        )
        total = result if total is None else total + result
    summed = lax.psum_scatter(
        total.astype(jnp.bfloat16), "ep", scatter_dimension=0, tiled=True
    )
    return lax.all_to_all(summed, "tp", split_axis=1, concat_axis=0, tiled=True).astype(jnp.float32)


def routed_sparse(own_rows, routing, route_weight, gate_weight, up_weight, down_weight, capacity):
    own_count = own_rows.shape[0]
    tp_index = lax.axis_index("tp")
    group_count, pick_count = routing.shape
    expert_count = lax.axis_size("ep") * gate_weight.shape[0]
    chosen, slot_ids = assign_slots(routing, own_count, capacity, expert_count)
    own_span = own_count * pick_count
    own_chosen = lax.dynamic_slice_in_dim(chosen, tp_index * own_span, own_span, 0)
    own_slots = (
        lax.dynamic_slice_in_dim(slot_ids, tp_index * own_span, own_span, 0) - tp_index * capacity
    )
    outgoing = gather_slots(own_rows, own_chosen, own_slots, capacity, expert_count, pick_count)
    arrived = lax.all_to_all(outgoing, "ep", split_axis=1, concat_axis=1, tiled=True)
    hidden = expert_hidden(
        lax.all_gather(arrived, "tp", axis=0, tiled=True), gate_weight, up_weight
    )
    full_hidden = lax.all_gather(hidden, "tp", axis=3, tiled=True)
    results = jnp.einsum(
        "snxf,xfe->snxe", full_hidden, down_weight, preferred_element_type=jnp.float32
    ).astype(jnp.bfloat16)
    results = results.reshape(results.shape[0], expert_count, results.shape[3])
    returned = lax.all_to_all(results, "ep", split_axis=1, concat_axis=1, tiled=True)
    flat_results = returned.reshape(returned.shape[0] * expert_count, returned.shape[2])
    picked = flat_results[slot_ids * expert_count + chosen].astype(jnp.float32)
    return jnp.sum(picked.reshape(group_count, pick_count, -1) * route_weight[:, :, None], axis=1)


def shards(
    mixer_input,
    expert_input,
    mixer_gain,
    expert_gain,
    query_weight,
    key_weight,
    value_weight,
    out_weight,
    decay_rate,
    routing,
    route_weight,
    gate_weight,
    up_weight,
    down_weight,
    shared_gate,
    shared_up,
    shared_down,
):
    own_count = mixer_input.shape[0]
    own_expert_rows = norm_rows(expert_input, expert_gain)
    mixer_rows, expert_rows = (
        lax.all_gather(norm_rows(mixer_input, mixer_gain), "tp", axis=0, tiled=True),
        lax.all_gather(own_expert_rows, "tp", axis=0, tiled=True),
    )
    group_count = mixer_rows.shape[0]
    head_total = decay_rate.shape[0]
    positions = (
        lax.axis_index("ep") * group_count + jnp.arange(group_count, dtype=jnp.int32)
    ).astype(jnp.float32)
    query_heads = rotate(project(mixer_rows, query_weight, head_total), positions) * HD ** (-0.5)
    key_heads = rotate(project(mixer_rows, key_weight, head_total), positions)
    value_heads = project(mixer_rows, value_weight, head_total)
    mixed_heads = retain_local(query_heads, key_heads, value_heads, decay_rate)
    mixer_output = lax.psum_scatter(
        jnp.dot(mixed_heads, out_weight, preferred_element_type=jnp.float32).astype(jnp.bfloat16),
        "tp",
        scatter_dimension=0,
        tiled=True,
    ).astype(jnp.float32)
    expert_count = lax.axis_size("ep") * gate_weight.shape[0]
    pick_count = routing.shape[1]
    capacity = (3 * own_count * pick_count + 2 * expert_count - 1) // (2 * expert_count)
    experts = (own_expert_rows, routing, route_weight, gate_weight, up_weight, down_weight)
    if 2 * capacity >= own_count:
        weighted = routed_dense(*experts)
    else:
        weighted = routed_sparse(*experts, capacity)
    shared_hidden = (
        jax.nn.silu(jnp.dot(expert_rows, shared_gate, preferred_element_type=jnp.float32))
        * jnp.dot(expert_rows, shared_up, preferred_element_type=jnp.float32)
    ).astype(jnp.bfloat16)
    full_shared = lax.all_gather(shared_hidden, "tp", axis=1, tiled=True)
    shared_result = jnp.dot(full_shared, shared_down, preferred_element_type=jnp.float32)
    expert_output = weighted + shared_result
    return (mixer_output, expert_output)


def solution(mesh):
    return jax.shard_map(
        shards,
        mesh=mesh,
        in_specs=(
            P(("ep", "tp"), None),
            P(("ep", "tp"), None),
            P(),
            P(),
            P(None, "tp"),
            P(None, "tp"),
            P(None, "tp"),
            P("tp", None),
            P("tp"),
            P("ep", None),
            P("ep", None),
            P("ep", None, "tp"),
            P("ep", None, "tp"),
            P("ep", None, "tp"),
            P(None, "tp"),
            P(None, "tp"),
            P(None, "tp"),
        ),
        out_specs=(P(("ep", "tp"), None), P("ep", "tp")),
        check_vma=False,
    )
```

```python
import jax
import jax.numpy as jnp
from jax import lax
from jax.sharding import PartitionSpec as P

HD = 128


NORM_EPS = 1e-06
ROPE_BASE = 10000.0


def swap(a, axis, bit):
    return lax.ppermute(a, axis, [(i, i ^ bit) for i in range(lax.axis_size(axis))])


def bits_of(axis):
    bits, bit = [], 1
    while bit < lax.axis_size(axis):
        bits.append(bit)
        bit *= 2
    return bits[::-1]


def gather_list(a, axis):
    held = {0: a}
    for bit in bits_of(axis):
        for k in list(held):
            held[k ^ bit] = swap(held[k], axis, bit)
    return [held[k] for k in range(len(held))]


def gather_small(a, axis):
    held = a[None]
    for bit in bits_of(axis)[::-1]:
        held = jnp.concatenate([held, swap(held, axis, bit)], axis=0)
    return held


def in_order(parts, axis, dim):
    me = lax.axis_index(axis)
    stacked = jnp.stack(parts)
    return jnp.concatenate(
        [
            lax.dynamic_index_in_dim(stacked, me ^ k, 0, keepdims=False)
            for k in range(len(parts))
        ],
        axis=dim,
    )


def scatter_sum(parts, axis, order):
    held = dict(enumerate(parts))
    for bit in order:
        for k in sorted(held, reverse=True):
            if k & bit:
                arrived = swap(held[k], axis, bit)
                held[k ^ bit] = (
                    held[k ^ bit].astype(jnp.float32) + arrived.astype(jnp.float32)
                ).astype(jnp.bfloat16)
                del held[k]
    return held[0]


def norm_rows(inputs, gain_vector):
    values = inputs.astype(jnp.float32)
    scaled = values * lax.rsqrt(jnp.mean(values * values, axis=-1, keepdims=True) + NORM_EPS)
    return (scaled * gain_vector).astype(jnp.bfloat16)


def rotate(head_rows, positions):
    head_size = head_rows.shape[-1]
    inverse = ROPE_BASE ** (-jnp.arange(0, head_size, 2, dtype=jnp.float32) / head_size)
    angles = positions[:, None] * inverse[None, :]
    cosine = jnp.cos(angles)[:, None, :]
    sine_part = jnp.sin(angles)[:, None, :]
    front_half = head_rows[..., : head_size // 2]
    behind = head_rows[..., head_size // 2 :]
    return jnp.concatenate(
        [front_half * cosine - behind * sine_part, front_half * sine_part + behind * cosine],
        axis=-1,
    )


def project(inputs, weight, head_total):
    product = jnp.dot(inputs, weight, preferred_element_type=jnp.float32).astype(jnp.bfloat16)
    product = lax.optimization_barrier(product)
    return product.astype(jnp.float32).reshape(inputs.shape[0], head_total, -1)


def retain_local(query_heads, key_heads, value_heads, decay_rates):
    length, head_total, head_size = query_heads.shape
    narrow = jnp.bfloat16
    log_gamma = -decay_rates
    place = lax.axis_index("ep")
    inner_pos = jnp.arange(length, dtype=jnp.float32)
    key_scale = jnp.exp(log_gamma[None, :] * (length - 1.0 - inner_pos)[:, None])
    summary = jnp.einsum(
        "nhd,nhe->hde",
        (key_heads * key_scale[:, :, None]).astype(narrow),
        value_heads.astype(narrow),
        preferred_element_type=jnp.float32,
    )
    gathered = gather_small(summary, "ep")
    gaps = (place - 1 - (place ^ jnp.arange(gathered.shape[0]))).astype(jnp.float32)
    mix = jnp.where(
        gaps[:, None] >= 0,
        jnp.exp(log_gamma[None, :] * length * jnp.maximum(gaps, 0.0)[:, None]),
        0.0,
    )
    incoming = jnp.sum(mix[:, :, None, None] * gathered, axis=0)
    offsets = inner_pos[:, None] - inner_pos[None, :]
    decay_mask = jnp.where(
        offsets >= 0, jnp.exp(log_gamma[:, None, None] * jnp.maximum(offsets, 0.0)), 0.0
    )
    scores = (
        jnp.einsum(
            "nhd,mhd->hnm",
            query_heads.astype(narrow),
            key_heads.astype(narrow),
            preferred_element_type=jnp.float32,
        )
        * decay_mask
    )
    nearby = jnp.einsum(
        "hnm,mhe->nhe",
        scores.astype(narrow),
        value_heads.astype(narrow),
        preferred_element_type=jnp.float32,
    )
    query_scale = jnp.exp(log_gamma[None, :] * (inner_pos + 1.0)[:, None])
    distant = jnp.einsum(
        "nhd,hde->nhe",
        (query_heads * query_scale[:, :, None]).astype(narrow),
        incoming.astype(narrow),
        preferred_element_type=jnp.float32,
    )
    retained = nearby + distant
    normed = retained * lax.rsqrt(jnp.mean(retained * retained, axis=-1, keepdims=True) + NORM_EPS)
    return normed.astype(jnp.bfloat16).reshape(length, head_total * head_size)


def assign_slots(routes, source_rows, capacity, expert_count):
    token_count, pick_count = routes.shape
    chosen = routes.reshape(token_count * pick_count)
    onehot = (chosen[:, None] == jnp.arange(expert_count, dtype=jnp.int32)[None, :]).astype(
        jnp.int32
    )
    per_source = onehot.reshape(token_count // source_rows, source_rows * pick_count, expert_count)
    earlier_hits = jnp.cumsum(per_source, axis=1) - per_source
    ranks = jnp.sum(earlier_hits * per_source, axis=2).reshape(token_count * pick_count)
    sources = jnp.arange(token_count * pick_count, dtype=jnp.int32) // (source_rows * pick_count)
    return (chosen, sources * capacity + ranks)


def gather_slots(token_rows, chosen, slot_ids, slot_count, expert_count, pick_count):
    owners = jnp.arange(chosen.shape[0], dtype=jnp.int32) // pick_count + 1
    owner_table = jnp.zeros((slot_count, expert_count), jnp.int32).at[slot_ids, chosen].set(owners)
    padded = jnp.concatenate(
        [jnp.zeros((1, token_rows.shape[1]), token_rows.dtype), token_rows], axis=0
    )
    return padded[owner_table]


def expert_hidden(routed_rows, gate_weight, up_weight):
    per_device = gate_weight.shape[0]
    grouped = routed_rows.reshape(
        routed_rows.shape[0], routed_rows.shape[1] // per_device, per_device, routed_rows.shape[2]
    )
    gate_part = jnp.einsum(
        "snxd,xdf->snxf", grouped, gate_weight, preferred_element_type=jnp.float32
    )
    up_part = jnp.einsum("snxd,xdf->snxf", grouped, up_weight, preferred_element_type=jnp.float32)
    return (jax.nn.silu(gate_part) * up_part).astype(jnp.bfloat16)


def routed_dense(own_rows, routing, route_weight, gate_weight, up_weight, down_weight):
    own_count = own_rows.shape[0]
    local_experts = gate_weight.shape[0]
    expert_count = lax.axis_size("ep") * local_experts
    start = lax.axis_index("tp") * own_count
    own_routing = lax.dynamic_slice_in_dim(routing, start, own_count, 0)
    own_weight = lax.dynamic_slice_in_dim(route_weight, start, own_count, 0)
    named = own_routing[:, :, None] == jnp.arange(expert_count, dtype=jnp.int32)
    spread = jnp.sum(jnp.where(named, own_weight[:, :, None], 0.0), axis=1)
    scales = gather_small(spread, "ep")
    scales = lax.dynamic_slice_in_dim(
        scales, lax.axis_index("ep") * local_experts, local_experts, 2
    )
    gate_parts = gather_list(gate_weight, "tp")
    up_parts = gather_list(up_weight, "tp")
    down_parts = gather_list(down_weight, "tp")
    row_parts = gather_list(own_rows, "ep")
    sums = [None] * len(row_parts)
    for low in range(len(row_parts) - 2, -1, -2):
        rows = jnp.concatenate(row_parts[low : low + 2], axis=0)
        scale = scales[low : low + 2].reshape(2 * own_count, local_experts)
        total = [None] * len(down_parts)
        for x in range(local_experts):
            hidden = in_order(
                [
                    (
                        jax.nn.silu(jnp.dot(rows, g[x], preferred_element_type=jnp.float32))
                        * jnp.dot(rows, u[x], preferred_element_type=jnp.float32)
                    ).astype(jnp.bfloat16)
                    for g, u in zip(gate_parts, up_parts)
                ],
                "tp",
                1,
            )
            for p, down in enumerate(down_parts):
                result = (
                    jnp.dot(hidden, down[x], preferred_element_type=jnp.float32)
                    * scale[:, x : x + 1]
                )
                total[p] = result if total[p] is None else total[p] + result
        joined = jnp.concatenate([t.astype(jnp.bfloat16) for t in total], axis=1)
        sums[low], sums[low + 1] = joined[:own_count], joined[own_count:]
    summed = scatter_sum(sums, "ep", bits_of("ep")[::-1])
    width = down_weight.shape[2]
    columns = [summed[:, p * width : (p + 1) * width] for p in range(len(down_parts))]
    columns = [columns[0]] + [swap(columns[p], "tp", p) for p in range(1, len(columns))]
    return in_order(columns, "tp", 0).astype(jnp.float32)


def routed_sparse(own_rows, routing, route_weight, gate_weight, up_weight, down_weight, capacity):
    own_count = own_rows.shape[0]
    tp_index = lax.axis_index("tp")
    group_count, pick_count = routing.shape
    expert_count = lax.axis_size("ep") * gate_weight.shape[0]
    chosen, slot_ids = assign_slots(routing, own_count, capacity, expert_count)
    own_span = own_count * pick_count
    own_chosen = lax.dynamic_slice_in_dim(chosen, tp_index * own_span, own_span, 0)
    own_slots = (
        lax.dynamic_slice_in_dim(slot_ids, tp_index * own_span, own_span, 0) - tp_index * capacity
    )
    outgoing = gather_slots(own_rows, own_chosen, own_slots, capacity, expert_count, pick_count)
    arrived = lax.all_to_all(outgoing, "ep", split_axis=1, concat_axis=1, tiled=True)
    hidden = expert_hidden(
        lax.all_gather(arrived, "tp", axis=0, tiled=True), gate_weight, up_weight
    )
    full_hidden = lax.all_gather(hidden, "tp", axis=3, tiled=True)
    results = jnp.einsum(
        "snxf,xfe->snxe", full_hidden, down_weight, preferred_element_type=jnp.float32
    ).astype(jnp.bfloat16)
    results = results.reshape(results.shape[0], expert_count, results.shape[3])
    returned = lax.all_to_all(results, "ep", split_axis=1, concat_axis=1, tiled=True)
    flat_results = returned.reshape(returned.shape[0] * expert_count, returned.shape[2])
    picked = flat_results[slot_ids * expert_count + chosen].astype(jnp.float32)
    return jnp.sum(picked.reshape(group_count, pick_count, -1) * route_weight[:, :, None], axis=1)


def shards(
    mixer_input,
    expert_input,
    mixer_gain,
    expert_gain,
    query_weight,
    key_weight,
    value_weight,
    out_weight,
    decay_rate,
    routing,
    route_weight,
    gate_weight,
    up_weight,
    down_weight,
    shared_gate,
    shared_up,
    shared_down,
):
    own_count = mixer_input.shape[0]
    own_expert_rows = norm_rows(expert_input, expert_gain)
    mixer_rows, expert_rows = (
        in_order(gather_list(norm_rows(mixer_input, mixer_gain), "tp"), "tp", 0),
        in_order(gather_list(own_expert_rows, "tp"), "tp", 0),
    )
    group_count = mixer_rows.shape[0]
    head_total = decay_rate.shape[0]
    positions = (
        lax.axis_index("ep") * group_count + jnp.arange(group_count, dtype=jnp.int32)
    ).astype(jnp.float32)
    query_heads = rotate(project(mixer_rows, query_weight, head_total), positions) * HD ** (-0.5)
    key_heads = rotate(project(mixer_rows, key_weight, head_total), positions)
    value_heads = project(mixer_rows, value_weight, head_total)
    mixed_heads = retain_local(query_heads, key_heads, value_heads, decay_rate)
    partial_out = jnp.dot(mixed_heads, out_weight, preferred_element_type=jnp.float32).astype(
        jnp.bfloat16
    )
    tp_place = lax.axis_index("tp")
    blocks = [
        lax.dynamic_slice_in_dim(partial_out, (tp_place ^ k) * own_count, own_count, 0)
        for k in range(lax.axis_size("tp"))
    ]
    mixer_output = scatter_sum(blocks, "tp", bits_of("tp")).astype(jnp.float32)
    expert_count = lax.axis_size("ep") * gate_weight.shape[0]
    pick_count = routing.shape[1]
    capacity = (3 * own_count * pick_count + 2 * expert_count - 1) // (2 * expert_count)
    experts = (own_expert_rows, routing, route_weight, gate_weight, up_weight, down_weight)
    if 2 * capacity >= own_count:
        weighted = routed_dense(*experts)
    else:
        weighted = routed_sparse(*experts, capacity)
    shared_hidden = (
        jax.nn.silu(jnp.dot(expert_rows, shared_gate, preferred_element_type=jnp.float32))
        * jnp.dot(expert_rows, shared_up, preferred_element_type=jnp.float32)
    ).astype(jnp.bfloat16)
    full_shared = in_order(gather_list(shared_hidden, "tp"), "tp", 1)
    shared_result = jnp.dot(full_shared, shared_down, preferred_element_type=jnp.float32)
    expert_output = weighted + shared_result
    return (mixer_output, expert_output)


def solution(mesh):
    return jax.shard_map(
        shards,
        mesh=mesh,
        in_specs=(
            P(("ep", "tp"), None),
            P(("ep", "tp"), None),
            P(),
            P(),
            P(None, "tp"),
            P(None, "tp"),
            P(None, "tp"),
            P("tp", None),
            P("tp"),
            P("ep", None),
            P("ep", None),
            P("ep", None, "tp"),
            P("ep", None, "tp"),
            P("ep", None, "tp"),
            P(None, "tp"),
            P(None, "tp"),
            P(None, "tp"),
        ),
        out_specs=(P(("ep", "tp"), None), P("ep", "tp")),
        check_vma=False,
    )
```

```python
import jax
import jax.numpy as jnp
from jax import lax
from jax.sharding import PartitionSpec as P

HD = 128


NORM_EPS = 1e-06
ROPE_BASE = 10000.0


def swap(a, axis, bit):
    return lax.ppermute(a, axis, [(i, i ^ bit) for i in range(lax.axis_size(axis))])


def bits_of(axis):
    bits, bit = [], 1
    while bit < lax.axis_size(axis):
        bits.append(bit)
        bit *= 2
    return bits[::-1]


def gather_list(a, axis):
    held = {0: a}
    for bit in bits_of(axis):
        for k in list(held):
            held[k ^ bit] = swap(held[k], axis, bit)
    return [held[k] for k in range(len(held))]


def gather_small(a, axis):
    held = a[None]
    for bit in bits_of(axis)[::-1]:
        held = jnp.concatenate([held, swap(held, axis, bit)], axis=0)
    return held


def in_order(parts, axis, dim):
    me = lax.axis_index(axis)
    stacked = jnp.stack(parts)
    return jnp.concatenate(
        [
            lax.dynamic_index_in_dim(stacked, me ^ k, 0, keepdims=False)
            for k in range(len(parts))
        ],
        axis=dim,
    )


def scatter_sum(parts, axis, order):
    held = dict(enumerate(parts))
    for bit in order:
        for k in sorted(held, reverse=True):
            if k & bit:
                arrived = swap(held[k], axis, bit)
                held[k ^ bit] = (
                    held[k ^ bit].astype(jnp.float32) + arrived.astype(jnp.float32)
                ).astype(jnp.bfloat16)
                del held[k]
    return held[0]


def norm_rows(inputs, gain_vector):
    values = inputs.astype(jnp.float32)
    scaled = values * lax.rsqrt(jnp.mean(values * values, axis=-1, keepdims=True) + NORM_EPS)
    return (scaled * gain_vector).astype(jnp.bfloat16)


def rotate(head_rows, positions):
    head_size = head_rows.shape[-1]
    inverse = ROPE_BASE ** (-jnp.arange(0, head_size, 2, dtype=jnp.float32) / head_size)
    angles = positions[:, None] * inverse[None, :]
    cosine = jnp.cos(angles)[:, None, :]
    sine_part = jnp.sin(angles)[:, None, :]
    front_half = head_rows[..., : head_size // 2]
    behind = head_rows[..., head_size // 2 :]
    return jnp.concatenate(
        [front_half * cosine - behind * sine_part, front_half * sine_part + behind * cosine],
        axis=-1,
    )


def project(inputs, weight, head_total):
    product = jnp.dot(inputs, weight, preferred_element_type=jnp.float32).astype(jnp.bfloat16)
    product = lax.optimization_barrier(product)
    return product.astype(jnp.float32).reshape(inputs.shape[0], head_total, -1)


def retain_local(query_heads, key_heads, value_heads, decay_rates):
    length, head_total, head_size = query_heads.shape
    narrow = jnp.bfloat16
    log_gamma = -decay_rates
    place = lax.axis_index("ep")
    inner_pos = jnp.arange(length, dtype=jnp.float32)
    key_scale = jnp.exp(log_gamma[None, :] * (length - 1.0 - inner_pos)[:, None])
    summary = jnp.einsum(
        "nhd,nhe->hde",
        (key_heads * key_scale[:, :, None]).astype(narrow),
        value_heads.astype(narrow),
        preferred_element_type=jnp.float32,
    )
    gathered = gather_small(summary, "ep")
    gaps = (place - 1 - (place ^ jnp.arange(gathered.shape[0]))).astype(jnp.float32)
    mix = jnp.where(
        gaps[:, None] >= 0,
        jnp.exp(log_gamma[None, :] * length * jnp.maximum(gaps, 0.0)[:, None]),
        0.0,
    )
    incoming = jnp.sum(mix[:, :, None, None] * gathered, axis=0)
    offsets = inner_pos[:, None] - inner_pos[None, :]
    decay_mask = jnp.where(
        offsets >= 0, jnp.exp(log_gamma[:, None, None] * jnp.maximum(offsets, 0.0)), 0.0
    )
    scores = (
        jnp.einsum(
            "nhd,mhd->hnm",
            query_heads.astype(narrow),
            key_heads.astype(narrow),
            preferred_element_type=jnp.float32,
        )
        * decay_mask
    )
    nearby = jnp.einsum(
        "hnm,mhe->nhe",
        scores.astype(narrow),
        value_heads.astype(narrow),
        preferred_element_type=jnp.float32,
    )
    query_scale = jnp.exp(log_gamma[None, :] * (inner_pos + 1.0)[:, None])
    distant = jnp.einsum(
        "nhd,hde->nhe",
        (query_heads * query_scale[:, :, None]).astype(narrow),
        incoming.astype(narrow),
        preferred_element_type=jnp.float32,
    )
    retained = nearby + distant
    normed = retained * lax.rsqrt(jnp.mean(retained * retained, axis=-1, keepdims=True) + NORM_EPS)
    return normed.astype(jnp.bfloat16).reshape(length, head_total * head_size)


def assign_slots(routes, source_rows, capacity, expert_count):
    token_count, pick_count = routes.shape
    chosen = routes.reshape(token_count * pick_count)
    onehot = (chosen[:, None] == jnp.arange(expert_count, dtype=jnp.int32)[None, :]).astype(
        jnp.int32
    )
    per_source = onehot.reshape(token_count // source_rows, source_rows * pick_count, expert_count)
    earlier_hits = jnp.cumsum(per_source, axis=1) - per_source
    ranks = jnp.sum(earlier_hits * per_source, axis=2).reshape(token_count * pick_count)
    sources = jnp.arange(token_count * pick_count, dtype=jnp.int32) // (source_rows * pick_count)
    return (chosen, sources * capacity + ranks)


def gather_slots(token_rows, chosen, slot_ids, slot_count, expert_count, pick_count):
    owners = jnp.arange(chosen.shape[0], dtype=jnp.int32) // pick_count + 1
    owner_table = jnp.zeros((slot_count, expert_count), jnp.int32).at[slot_ids, chosen].set(owners)
    padded = jnp.concatenate(
        [jnp.zeros((1, token_rows.shape[1]), token_rows.dtype), token_rows], axis=0
    )
    return padded[owner_table]


def expert_hidden(routed_rows, gate_weight, up_weight):
    per_device = gate_weight.shape[0]
    grouped = routed_rows.reshape(
        routed_rows.shape[0], routed_rows.shape[1] // per_device, per_device, routed_rows.shape[2]
    )
    gate_part = jnp.einsum(
        "snxd,xdf->snxf", grouped, gate_weight, preferred_element_type=jnp.float32
    )
    up_part = jnp.einsum("snxd,xdf->snxf", grouped, up_weight, preferred_element_type=jnp.float32)
    return (jax.nn.silu(gate_part) * up_part).astype(jnp.bfloat16)


def routed_dense(own_rows, routing, route_weight, gate_weight, up_weight, down_weight):
    own_count = own_rows.shape[0]
    local_experts = gate_weight.shape[0]
    expert_count = lax.axis_size("ep") * local_experts
    start = lax.axis_index("tp") * own_count
    own_routing = lax.dynamic_slice_in_dim(routing, start, own_count, 0)
    own_weight = lax.dynamic_slice_in_dim(route_weight, start, own_count, 0)
    named = own_routing[:, :, None] == jnp.arange(expert_count, dtype=jnp.int32)
    spread = jnp.sum(jnp.where(named, own_weight[:, :, None], 0.0), axis=1)
    gate_parts = gather_list(gate_weight, "tp")
    up_parts = gather_list(up_weight, "tp")
    down_parts = gather_list(down_weight, "tp")
    model = own_rows.shape[1]
    upper = spread.astype(jnp.bfloat16)
    lower = (spread - upper.astype(jnp.float32)).astype(jnp.bfloat16)
    row_parts = gather_list(jnp.concatenate([own_rows, upper, lower], axis=1), "ep")
    rows = jnp.concatenate([part[:, :model] for part in row_parts], axis=0)
    tails = jnp.concatenate([part[:, model:] for part in row_parts], axis=0).astype(jnp.float32)
    scales = lax.dynamic_slice_in_dim(
        tails[:, :expert_count] + tails[:, expert_count:],
        lax.axis_index("ep") * local_experts,
        local_experts,
        1,
    )
    hiddens = [
        in_order(
            [
                (
                    jax.nn.silu(jnp.dot(rows, g[x], preferred_element_type=jnp.float32))
                    * jnp.dot(rows, u[x], preferred_element_type=jnp.float32)
                ).astype(jnp.bfloat16)
                for g, u in zip(gate_parts, up_parts)
            ],
            "tp",
            1,
        )
        for x in range(local_experts)
    ]
    sums = [None] * len(row_parts)
    group = max(len(row_parts) // 2, 1)
    for low in range(len(row_parts) - group, -1, -group):
        span = slice(low * own_count, (low + group) * own_count)
        total = [None] * len(down_parts)
        for x in range(local_experts):
            for p, down in enumerate(down_parts):
                result = (
                    jnp.dot(hiddens[x][span], down[x], preferred_element_type=jnp.float32)
                    * scales[span, x : x + 1]
                )
                total[p] = result if total[p] is None else total[p] + result
        joined = jnp.concatenate([t.astype(jnp.bfloat16) for t in total], axis=1)
        for k in range(group):
            sums[low + k] = joined[k * own_count : (k + 1) * own_count]
    summed = scatter_sum(sums, "ep", bits_of("ep")[::-1])
    width = down_weight.shape[2]
    columns = [summed[:, p * width : (p + 1) * width] for p in range(len(down_parts))]
    columns = [columns[0]] + [swap(columns[p], "tp", p) for p in range(1, len(columns))]
    return in_order(columns, "tp", 0).astype(jnp.float32)


def routed_sparse(own_rows, routing, route_weight, gate_weight, up_weight, down_weight, capacity):
    own_count = own_rows.shape[0]
    tp_index = lax.axis_index("tp")
    group_count, pick_count = routing.shape
    expert_count = lax.axis_size("ep") * gate_weight.shape[0]
    chosen, slot_ids = assign_slots(routing, own_count, capacity, expert_count)
    own_span = own_count * pick_count
    own_chosen = lax.dynamic_slice_in_dim(chosen, tp_index * own_span, own_span, 0)
    own_slots = (
        lax.dynamic_slice_in_dim(slot_ids, tp_index * own_span, own_span, 0) - tp_index * capacity
    )
    outgoing = gather_slots(own_rows, own_chosen, own_slots, capacity, expert_count, pick_count)
    arrived = lax.all_to_all(outgoing, "ep", split_axis=1, concat_axis=1, tiled=True)
    hidden = expert_hidden(
        lax.all_gather(arrived, "tp", axis=0, tiled=True), gate_weight, up_weight
    )
    full_hidden = lax.all_gather(hidden, "tp", axis=3, tiled=True)
    results = jnp.einsum(
        "snxf,xfe->snxe", full_hidden, down_weight, preferred_element_type=jnp.float32
    ).astype(jnp.bfloat16)
    results = results.reshape(results.shape[0], expert_count, results.shape[3])
    returned = lax.all_to_all(results, "ep", split_axis=1, concat_axis=1, tiled=True)
    flat_results = returned.reshape(returned.shape[0] * expert_count, returned.shape[2])
    picked = flat_results[slot_ids * expert_count + chosen].astype(jnp.float32)
    return jnp.sum(picked.reshape(group_count, pick_count, -1) * route_weight[:, :, None], axis=1)


def shards(
    mixer_input,
    expert_input,
    mixer_gain,
    expert_gain,
    query_weight,
    key_weight,
    value_weight,
    out_weight,
    decay_rate,
    routing,
    route_weight,
    gate_weight,
    up_weight,
    down_weight,
    shared_gate,
    shared_up,
    shared_down,
):
    own_count = mixer_input.shape[0]
    own_expert_rows = norm_rows(expert_input, expert_gain)
    both_rows = in_order(
        gather_list(jnp.stack([norm_rows(mixer_input, mixer_gain), own_expert_rows]), "tp"),
        "tp",
        1,
    )
    mixer_rows, expert_rows = both_rows[0], both_rows[1]
    group_count = mixer_rows.shape[0]
    head_total = decay_rate.shape[0]
    positions = (
        lax.axis_index("ep") * group_count + jnp.arange(group_count, dtype=jnp.int32)
    ).astype(jnp.float32)
    query_heads = rotate(project(mixer_rows, query_weight, head_total), positions) * HD ** (-0.5)
    key_heads = rotate(project(mixer_rows, key_weight, head_total), positions)
    value_heads = project(mixer_rows, value_weight, head_total)
    mixed_heads = retain_local(query_heads, key_heads, value_heads, decay_rate)
    partial_out = jnp.dot(mixed_heads, out_weight, preferred_element_type=jnp.float32).astype(
        jnp.bfloat16
    )
    tp_place = lax.axis_index("tp")
    blocks = [
        lax.dynamic_slice_in_dim(partial_out, (tp_place ^ k) * own_count, own_count, 0)
        for k in range(lax.axis_size("tp"))
    ]
    mixer_output = scatter_sum(blocks, "tp", bits_of("tp")).astype(jnp.float32)
    expert_count = lax.axis_size("ep") * gate_weight.shape[0]
    pick_count = routing.shape[1]
    capacity = (3 * own_count * pick_count + 2 * expert_count - 1) // (2 * expert_count)
    experts = (own_expert_rows, routing, route_weight, gate_weight, up_weight, down_weight)
    if 2 * capacity >= own_count:
        weighted = routed_dense(*experts)
    else:
        weighted = routed_sparse(*experts, capacity)
    shared_hidden = (
        jax.nn.silu(jnp.dot(expert_rows, shared_gate, preferred_element_type=jnp.float32))
        * jnp.dot(expert_rows, shared_up, preferred_element_type=jnp.float32)
    ).astype(jnp.bfloat16)
    full_shared = in_order(gather_list(shared_hidden, "tp"), "tp", 1)
    shared_result = jnp.dot(full_shared, shared_down, preferred_element_type=jnp.float32)
    expert_output = weighted + shared_result
    return (mixer_output, expert_output)


def solution(mesh):
    return jax.shard_map(
        shards,
        mesh=mesh,
        in_specs=(
            P(("ep", "tp"), None),
            P(("ep", "tp"), None),
            P(),
            P(),
            P(None, "tp"),
            P(None, "tp"),
            P(None, "tp"),
            P("tp", None),
            P("tp"),
            P("ep", None),
            P("ep", None),
            P("ep", None, "tp"),
            P("ep", None, "tp"),
            P("ep", None, "tp"),
            P(None, "tp"),
            P(None, "tp"),
            P(None, "tp"),
        ),
        out_specs=(P(("ep", "tp"), None), P("ep", "tp")),
        check_vma=False,
    )
```
